32 devices in a mesh: ep: 32 (over z, y, x, core).
Axes of the slice: x: 2, y: 2, z: 4, core: 2. Of those that a mesh axis runs over, the one named last changes fastest.
Arguments:
- tokens: bfloat16 [1536, 2048], P('ep'), may hold values from -6 to 6
- history_length: int32 [1536], P('ep'), may hold values from 1024 to 8192
- norm_gain: float32 [2048], replicated, may hold values from 0.1 to 1.9
- w_query: bfloat16 [2048, 512], replicated, may hold values from -0.125 to 0.125
- w_key: bfloat16 [2048, 512], replicated, may hold values from -0.125 to 0.125
- w_value: bfloat16 [2048, 512], replicated, may hold values from -0.125 to 0.125
- w_gate: bfloat16 [2048, 512], replicated, may hold values from -0.125 to 0.125
- decay_rate: float32 [8], replicated, may hold values from 0.003 to 0.7
- state: float32 [1536, 8, 64, 64], P('ep'), may hold values from -4 to 4
- head_gain: float32 [512], replicated, may hold values from 0.1 to 1.9
- w_out: bfloat16 [512, 2048], replicated, may hold values from -0.25 to 0.25
- moe_gain: float32 [2048], replicated, may hold values from 0.1 to 1.9
- route_weights: float32 [1536, 2], P('ep'), may hold values from 0.3 to 3
- expert_group: int32 [1536], P('ep'), may hold values from 0 to 3, as said below
- expert_inner: int32 [1536, 2], P('ep'), may hold values from 0 to 7, as said below
- expert_gate: bfloat16 [32, 2048, 256], P('ep'), may hold values from -0.125 to 0.125
- expert_up: bfloat16 [32, 2048, 256], P('ep'), may hold values from -0.125 to 0.125
- expert_down: bfloat16 [32, 256, 2048], P('ep'), may hold values from -0.375 to 0.375
Outputs:
- output: bfloat16 [1536, 2048], P('ep')
- new_state: float32 [1536, 8, 64, 64], P('ep')
The draws below stay inside these ranges and needn't reach their ends.
Inputs may be any that keep to these rules, and one draw needn't show every extreme that they name: `expert_group`: together with expert_inner it names 2 different experts of one group for each token. `expert_inner`: the rows of one device name one expert at most 6 times; in every draw some expert is named exactly 6 times by the rows of every device.
All inputs are finite; a program needn't handle non-finite values.
Results may differ from the reference program's by a relative error of at most 0.02.
Values may be sent and summed in bfloat16 or wider, within the bound.
A program may use at most 128 MiB of HBM per device.

```python
import math
import jax
import jax.numpy as jnp
from jax import lax

D = 2048
HEADS = 8
HEAD_DIM = 64
RET_WIDTH = 512
EXPERT_WIDTH = 256
SEQ_DEV = 48
TOKENS = 1536
EXPERTS = 32
GROUPS = 4
GROUP_SIZE = 8
TOP_K = 2
CAP = 6
N_EP = 32


def route_table(key):
    root_key = jax.random.fold_in(key, 7)
    pair_count = EXPERTS * CAP // 2
    per_group = pair_count // GROUPS
    hot_group = jax.random.randint(jax.random.fold_in(root_key, 1), (), 0, GROUPS)
    relabel = jax.vmap(lambda subkey: jax.random.permutation(subkey, GROUP_SIZE))(jax.random.split(jax.random.fold_in(root_key, 2), GROUPS))
    pair_ids = jnp.arange(pair_count, dtype=jnp.int32)
    pair_group = pair_ids // per_group
    pair_offset = pair_ids % per_group
    first_inner = relabel[pair_group, 2 * pair_offset % GROUP_SIZE]
    second_inner = relabel[pair_group, (2 * pair_offset + 1) % GROUP_SIZE]
    heated = (pair_group == hot_group) & (pair_offset % (GROUP_SIZE // 2) == 0)

    def one_block(subkey):
        jitter = jax.random.randint(jax.random.fold_in(subkey, 1), (pair_count,), 0, 1 << 20)
        scores = jnp.where(heated, pair_ids, (jitter + 1) * pair_count + pair_ids)
        _, chosen = lax.top_k(-scores, SEQ_DEV)
        chosen = chosen[jax.random.permutation(jax.random.fold_in(subkey, 2), SEQ_DEV)]
        return (pair_group[chosen], jnp.stack([first_inner[chosen], second_inner[chosen]], axis=-1))
    groups, inner_ids = jax.vmap(one_block)(jax.random.split(jax.random.fold_in(root_key, 3), TOKENS // SEQ_DEV))
    return (groups.reshape(TOKENS).astype(jnp.int32), inner_ids.reshape(TOKENS, TOP_K).astype(jnp.int32))


def draw_expert_group(key, part):
    return route_table(key)[0]


def draw_expert_inner(key, part):
    return route_table(key)[1]


def place_ends(result, own_key, least, largest):
    dims = result.shape
    index_at = [jax.random.randint(jax.random.fold_in(own_key, axis), (), 0, dims[axis]) for axis in range(len(dims))]
    result = result.at[tuple(index_at)].set(least)
    longest = dims.index(max(dims))
    index_at[longest] = (index_at[longest] + 1) % dims[longest]
    return result.at[tuple(index_at)].set(largest)


def block_levels(own_key, extent, cuts, low, high):
    level = 1.0
    for position, shards_of in cuts:
        steps = jax.random.uniform(jax.random.fold_in(jax.random.fold_in(own_key, 6), position), (shards_of,), jnp.float32, low / len(cuts), high / len(cuts))
        level = level * jnp.repeat(jnp.exp(steps), extent[position] // shards_of).reshape((-1,) + (1,) * (len(extent) - 1 - position))
    return level


def normal_values(own_key, extent, scale, most, cuts=(), held_as=jnp.bfloat16):
    values = scale * jax.random.normal(own_key, extent, jnp.float32)
    if cuts:
        values = values * block_levels(own_key, extent, cuts, -0.22, 0.18)
    return jnp.clip(values, -most, most).astype(held_as)


def setup_inputs(seed: int = 0) -> dict:
    key_list = jax.random.split(jax.random.key(seed), 19)
    return {
        "tokens": normal_values(key_list[0], (TOKENS, D), 1.0, 6.0, ((0, 32),)),
        "history_length": place_ends(jax.random.randint(key_list[1], (TOKENS,), 1024, 8193), jax.random.fold_in(key_list[1], 1), 1024, 8192).astype(jnp.int32),
        "norm_gain": jnp.clip(1.0 + 0.18 * jax.random.normal(key_list[2], (D,), jnp.float32), 0.1, 1.9),
        "w_query": normal_values(key_list[3], (D, RET_WIDTH), D ** -0.5, 0.125),
        "w_key": normal_values(key_list[4], (D, RET_WIDTH), D ** -0.5, 0.125),
        "w_value": normal_values(key_list[5], (D, RET_WIDTH), D ** -0.5, 0.125),
        "w_gate": normal_values(key_list[6], (D, RET_WIDTH), D ** -0.5, 0.125),
        "decay_rate": jnp.clip(jnp.exp(jax.random.uniform(key_list[7], (HEADS,), jnp.float32, math.log(0.003), math.log(0.7))), 0.003, 0.7),
        "state": normal_values(key_list[8], (TOKENS, HEADS, HEAD_DIM, HEAD_DIM), 0.3, 4.0, ((0, 32),), jnp.float32),
        "head_gain": jnp.clip(1.0 + 0.18 * jax.random.normal(key_list[9], (RET_WIDTH,), jnp.float32), 0.1, 1.9),
        "w_out": normal_values(key_list[10], (RET_WIDTH, D), RET_WIDTH ** -0.5, 0.25),
        "moe_gain": jnp.clip(1.0 + 0.18 * jax.random.normal(key_list[11], (D,), jnp.float32), 0.1, 1.9),
        "route_weights": jnp.clip(jnp.exp(math.log(3.0) - 2.3025851 * jax.random.uniform(key_list[12], (TOKENS, TOP_K), jnp.float32) ** block_levels(key_list[12], (TOKENS, TOP_K), ((0, 32),), -0.2, 0.2)), 0.3, 3.0),
        "expert_group": draw_expert_group(jax.random.fold_in(key_list[18], 71), 0),
        "expert_inner": draw_expert_inner(jax.random.fold_in(key_list[18], 71), 0),
        "expert_gate": normal_values(key_list[15], (EXPERTS, D, EXPERT_WIDTH), D ** -0.5, 0.125, ((0, 32),)),
        "expert_up": normal_values(key_list[16], (EXPERTS, D, EXPERT_WIDTH), D ** -0.5, 0.125, ((0, 32),)),
        "expert_down": normal_values(key_list[17], (EXPERTS, EXPERT_WIDTH, D), EXPERT_WIDTH ** -0.5, 0.375, ((0, 32),)),
    }


epsilon = 1e-06

def rotate(values, places):
    halfway = values.shape[-1] // 2
    inverse = 10000.0 ** (-jnp.arange(halfway, dtype=jnp.float32) / halfway)
    angles = places[:, None] * inverse[None, :]
    cosine = jnp.cos(angles)[:, None, :]
    sine_table = jnp.sin(angles)[:, None, :]
    first_half = values[..., :halfway]
    second = values[..., halfway:]
    return jnp.concatenate([first_half * cosine - second * sine_table, first_half * sine_table + second * cosine], axis=-1)

def rms_scale(values, gains):
    return values * lax.rsqrt(lax.optimization_barrier(jnp.mean(values * values, axis=-1, keepdims=True)) + epsilon) * gains

def retention_step(tokens, history_length, norm_gain, w_query, w_key, w_value, w_gate, decay_rate, state, head_gain, w_out, moe_gain):
    row_count = tokens.shape[0]
    head_count = decay_rate.shape[0]
    head_width = state.shape[-1]
    inputs = tokens.astype(jnp.float32)
    normed = rms_scale(inputs, norm_gain).astype(jnp.bfloat16)

    def project(weights):
        return jnp.dot(normed, weights, preferred_element_type=jnp.float32).astype(jnp.bfloat16)
    queries = project(w_query).reshape(row_count, head_count, head_width).astype(jnp.float32)
    keys_now = project(w_key).reshape(row_count, head_count, head_width).astype(jnp.float32)
    values_now = project(w_value).reshape(row_count, head_count, head_width).astype(jnp.float32)
    gating = project(w_gate).astype(jnp.float32)
    places = history_length.astype(jnp.float32)
    queries = rotate(queries, places)
    keys_now = rotate(keys_now, places) * head_width ** (-0.5)
    retain = jnp.exp(-decay_rate)
    new_state = retain[None, :, None, None] * state + keys_now[:, :, :, None] * values_now[:, :, None, :]
    reading = jnp.einsum('bhk,bhkv->bhv', queries, new_state, precision=lax.Precision.HIGHEST)
    reading = rms_scale(reading, head_gain.reshape(head_count, head_width))
    mixed_heads = (reading.reshape(row_count, head_count * head_width) * jax.nn.silu(gating)).astype(jnp.bfloat16)
    mixed_tokens = (inputs + jnp.dot(mixed_heads, w_out, preferred_element_type=jnp.float32)).astype(jnp.bfloat16)
    normed_moe = rms_scale(mixed_tokens.astype(jnp.float32), moe_gain).astype(jnp.bfloat16)
    return (mixed_tokens, normed_moe, new_state)

def expert_apply(row_block, gate_weight, up_weight, down_weight):
    gate_part = jnp.dot(row_block, gate_weight, preferred_element_type=jnp.float32)
    up_part = jnp.dot(row_block, up_weight, preferred_element_type=jnp.float32)
    hidden = (jax.nn.silu(gate_part) * up_part).astype(jnp.bfloat16)
    return jnp.dot(hidden, down_weight, preferred_element_type=jnp.float32).astype(jnp.bfloat16)

def reference(tokens, history_length, norm_gain, w_query, w_key, w_value, w_gate, decay_rate, state, head_gain, w_out, moe_gain, route_weights, expert_group, expert_inner, expert_gate, expert_up, expert_down):
    mixed_tokens, normed_moe, new_state = retention_step(tokens, history_length, norm_gain, w_query, w_key, w_value, w_gate, decay_rate, state, head_gain, w_out, moe_gain)
    row_count = tokens.shape[0]
    experts = expert_gate.shape[0]
    per_group = experts // GROUPS
    flat_ids = (expert_group[:, None] * per_group + expert_inner).reshape(-1).astype(jnp.int32)
    slot_total = flat_ids.shape[0]
    padded_ids = jnp.concatenate([flat_ids, jnp.full((1,), -1, jnp.int32)])
    owners = jnp.concatenate([jnp.arange(slot_total, dtype=jnp.int32) // TOP_K, jnp.zeros((1,), jnp.int32)])
    scales = jnp.concatenate([route_weights.reshape(-1), jnp.zeros((1,), jnp.float32)])
    row_bound = N_EP * CAP

    def visit_expert(running, expert):
        matched = padded_ids == expert
        picked = jnp.nonzero(matched, size=row_bound, fill_value=slot_total)[0].astype(jnp.int32)
        owner_rows = owners[picked]
        weighting = jnp.where(matched[picked], scales[picked], jnp.zeros_like(scales[picked]))
        outputs = expert_apply(normed_moe[owner_rows], expert_gate[expert], expert_up[expert], expert_down[expert])
        running = running.at[owner_rows].add(outputs.astype(jnp.float32) * weighting[:, None])
        return (running, None)
    running, _ = lax.scan(visit_expert, jnp.zeros((row_count, tokens.shape[1]), jnp.float32), jnp.arange(experts, dtype=jnp.int32))
    output = (mixed_tokens.astype(jnp.float32) + running).astype(jnp.bfloat16)
    return (output, new_state)
```

```python
import jax
import jax.numpy as jnp
from jax import lax
from jax.experimental import pallas as pl
from jax.experimental.pallas import tpu as pltpu
from jax.sharding import PartitionSpec as P

GROUPS = 4
TOP_K = 2


epsilon = 1e-06


def rotate(values, places):
    halfway = values.shape[-1] // 2
    inverse = 10000.0 ** (-jnp.arange(halfway, dtype=jnp.float32) / halfway)
    angles = places[:, None] * inverse[None, :]
    cosine = jnp.cos(angles)[:, None, :]
    sine_table = jnp.sin(angles)[:, None, :]
    first_half = values[..., :halfway]
    second = values[..., halfway:]
    return jnp.concatenate(
        [first_half * cosine - second * sine_table, first_half * sine_table + second * cosine],
        axis=-1,
    )


def rms_scale(values, gains):
    return values * lax.rsqrt(jnp.mean(values * values, axis=-1, keepdims=True) + epsilon) * gains


def retention_step(
    tokens,
    history_length,
    norm_gain,
    w_query,
    w_key,
    w_value,
    w_gate,
    decay_rate,
    state,
    head_gain,
    w_out,
    moe_gain,
):
    row_count = tokens.shape[0]
    head_count = decay_rate.shape[0]
    head_width = state.shape[-1]
    inputs = tokens.astype(jnp.float32)
    normed = rms_scale(inputs, norm_gain).astype(jnp.bfloat16)

    def project(weights):
        return jnp.dot(normed, weights, preferred_element_type=jnp.float32).astype(jnp.bfloat16)

    queries = project(w_query).reshape(row_count, head_count, head_width).astype(jnp.float32)
    keys_now = project(w_key).reshape(row_count, head_count, head_width).astype(jnp.float32)
    values_now = project(w_value).reshape(row_count, head_count, head_width).astype(jnp.float32)
    gating = project(w_gate).astype(jnp.float32)
    places = history_length.astype(jnp.float32)
    queries = rotate(queries, places)
    keys_now = rotate(keys_now, places) * head_width ** (-0.5)
    retain = jnp.exp(-decay_rate)
    new_state = (
        retain[None, :, None, None] * state + keys_now[:, :, :, None] * values_now[:, :, None, :]
    )
    reading = jnp.einsum("bhk,bhkv->bhv", queries, new_state, precision=lax.Precision.HIGHEST)
    reading = rms_scale(reading, head_gain.reshape(head_count, head_width))
    mixed_heads = (
        reading.reshape(row_count, head_count * head_width) * jax.nn.silu(gating)
    ).astype(jnp.bfloat16)
    mixed_tokens = (
        inputs + jnp.dot(mixed_heads, w_out, preferred_element_type=jnp.float32)
    ).astype(jnp.bfloat16)
    normed_moe = rms_scale(mixed_tokens.astype(jnp.float32), moe_gain).astype(jnp.bfloat16)
    return (mixed_tokens, normed_moe, new_state)


MESH = pl.DeviceIdType.MESH
CHUNKS = 4


def dot(a, b):
    return jnp.dot(a, b, preferred_element_type=jnp.float32)


def exchange_kernel(
    per_group,
    normed,
    mixed,
    place,
    collect,
    token_meta,
    gate_hbm,
    up_hbm,
    down_hbm,
    out,
    gate_w,
    up_w,
    down_w,
    meta_send,
    meta_recv,
    zsend,
    zrecv,
    dsend,
    drecv,
    osend,
    orecv,
    csend,
    crecv,
    load_sem,
    meta_sems,
    z_sems,
    d_sems,
    o_sems,
    c_sems,
):
    device = lax.axis_index("ep")
    group = device // per_group
    inner = device % per_group
    width = zsend.shape[-1]
    group_rows = zsend.shape[2]
    peer_rows = dsend.shape[2]
    slots = GROUPS * group_rows
    rows = per_group * peer_rows

    def column_peer(step):
        other = lax.rem(group + step, GROUPS)
        return other, other * per_group + inner

    def plane_peer(step):
        other = lax.rem(inner + step, per_group)
        return other, group * per_group + other

    def column_copy(source, target, sems, chunk, step):
        other, peer = column_peer(step)
        return pltpu.make_async_remote_copy(
            src_ref=source.at[chunk, other],
            dst_ref=target.at[chunk, group],
            send_sem=sems.at[0, chunk, step],
            recv_sem=sems.at[1, chunk, step],
            device_id=(peer,),
            device_id_type=MESH,
        )

    def plane_copy(source, target, sems, chunk, step):
        other, peer = plane_peer(step)
        return pltpu.make_async_remote_copy(
            src_ref=source.at[chunk, other],
            dst_ref=target.at[chunk, inner],
            send_sem=sems.at[0, chunk, step],
            recv_sem=sems.at[1, chunk, step],
            device_id=(peer,),
            device_id_type=MESH,
        )

    def meta_copy(step):
        other, peer = column_peer(step)
        return pltpu.make_async_remote_copy(
            src_ref=meta_send.at[other],
            dst_ref=meta_recv.at[group],
            send_sem=meta_sems.at[0, step],
            recv_sem=meta_sems.at[1, step],
            device_id=(peer,),
            device_id_type=MESH,
        )

    def each_column(act):
        for step in (2, 1, 3):
            act(step)

    def each_plane(act):
        def body(step, carry):
            act(step)
            return carry

        lax.fori_loop(1, per_group, body, 0)

    loads = [
        pltpu.make_async_copy(source, target, load_sem.at[place_index])
        for place_index, (source, target) in enumerate(
            ((gate_hbm, gate_w), (up_hbm, up_w), (down_hbm, down_w))
        )
    ]
    for load in loads:
        load.start()
    barrier = pltpu.get_barrier_semaphore()

    def greet_column(step):
        pl.semaphore_signal(barrier, inc=1, device_id=(column_peer(step)[1],), device_id_type=MESH)

    def greet_plane(step):
        pl.semaphore_signal(barrier, inc=1, device_id=(plane_peer(step)[1],), device_id_type=MESH)

    each_column(greet_column)
    each_plane(greet_plane)
    placing = place[...]
    meta = dot(placing, token_meta[...]).astype(jnp.bfloat16)
    meta_send[...] = meta.reshape(meta_send.shape)
    for chunk in range(CHUNKS):
        columns = slice(chunk * width, (chunk + 1) * width)
        block = dot(placing, normed[:, columns]).astype(jnp.bfloat16)
        zsend[chunk] = block.reshape(zsend.shape[1:])
    pl.semaphore_wait(barrier, GROUPS - 1 + per_group - 1)
    each_column(lambda step: meta_copy(step).start())
    for chunk in range(CHUNKS):
        each_column(lambda step: column_copy(zsend, zrecv, z_sems, chunk, step).start())
    meta_recv[group] = meta_send[group]
    for chunk in range(CHUNKS):
        zrecv[chunk, group] = zsend[chunk, group]
    each_column(lambda step: meta_copy(step).wait_recv())
    meta = meta_recv[...].reshape(slots, meta_recv.shape[-1]).astype(jnp.float32)
    row_ids = lax.broadcasted_iota(jnp.int32, (slots, rows), 1).astype(jnp.float32) + 1.0
    first = (row_ids == meta[:, 0:1]).astype(jnp.float32)
    second = (row_ids == meta[:, 1:2]).astype(jnp.float32)
    spread = (first + second).astype(jnp.bfloat16)
    weights = first * (meta[:, 2:3] + meta[:, 3:4]) + second * (meta[:, 4:5] + meta[:, 5:6])
    weights_high = weights.astype(jnp.bfloat16)
    weights_low = (weights - weights_high.astype(jnp.float32)).astype(jnp.bfloat16)
    for chunk in range(CHUNKS):
        each_column(lambda step: column_copy(zsend, zrecv, z_sems, chunk, step).wait_recv())
        block = lax.dot_general(
            spread,
            zrecv[chunk].reshape(slots, width),
            (((0,), (0,)), ((), ())),
            preferred_element_type=jnp.float32,
        ).astype(jnp.bfloat16)
        dsend[chunk] = block.reshape(dsend.shape[1:])
        each_plane(lambda step: plane_copy(dsend, drecv, d_sems, chunk, step).start())
        drecv[chunk, inner] = dsend[chunk, inner]
    loads[0].wait()
    loads[1].wait()
    loads[2].wait()
    gate_part = jnp.zeros((rows, gate_w.shape[1]), jnp.float32)
    up_part = jnp.zeros((rows, gate_w.shape[1]), jnp.float32)
    for chunk in range(CHUNKS):
        columns = slice(chunk * width, (chunk + 1) * width)
        each_plane(lambda step: plane_copy(dsend, drecv, d_sems, chunk, step).wait_recv())
        block = drecv[chunk].reshape(rows, width)
        gate_part += dot(block, gate_w[columns, :])
        up_part += dot(block, up_w[columns, :])
    hidden = (jax.nn.silu(gate_part) * up_part).astype(jnp.bfloat16)
    for chunk in range(CHUNKS):
        columns = slice(chunk * width, (chunk + 1) * width)
        block = dot(hidden, down_w[:, columns]).astype(jnp.bfloat16)
        osend[chunk] = block.reshape(osend.shape[1:])
        each_plane(lambda step: plane_copy(osend, orecv, o_sems, chunk, step).start())
        orecv[chunk, inner] = osend[chunk, inner]
    for chunk in range(CHUNKS):
        each_plane(lambda step: plane_copy(osend, orecv, o_sems, chunk, step).wait_recv())
        block = orecv[chunk].reshape(rows, width)
        block = (dot(weights_high, block) + dot(weights_low, block)).astype(jnp.bfloat16)
        csend[chunk] = block.reshape(csend.shape[1:])
        each_column(lambda step: column_copy(csend, crecv, c_sems, chunk, step).start())
        crecv[chunk, group] = csend[chunk, group]
    collecting = collect[...]
    for chunk in range(CHUNKS):
        columns = slice(chunk * width, (chunk + 1) * width)
        each_column(lambda step: column_copy(csend, crecv, c_sems, chunk, step).wait_recv())
        block = dot(collecting, crecv[chunk].reshape(slots, width))
        out[:, columns] = (mixed[:, columns].astype(jnp.float32) + block).astype(jnp.bfloat16)
    each_column(lambda step: meta_copy(step).wait_send())

    def drain(chunk, carry):
        each_column(lambda step: column_copy(zsend, zrecv, z_sems, chunk, step).wait_send())
        each_column(lambda step: column_copy(csend, crecv, c_sems, chunk, step).wait_send())
        each_plane(lambda step: plane_copy(dsend, drecv, d_sems, chunk, step).wait_send())
        each_plane(lambda step: plane_copy(osend, orecv, o_sems, chunk, step).wait_send())
        return carry

    lax.fori_loop(0, CHUNKS, drain, 0)


def earlier_equal(ids):
    count = ids.shape[0]
    before = jnp.arange(count)[:, None] > jnp.arange(count)[None, :]
    return jnp.sum((ids[:, None] == ids[None, :]) & before, axis=1).astype(jnp.int32)


def routed_experts(
    mixed_tokens, normed_moe, route_weights, expert_group, expert_inner, expert_gate, expert_up, expert_down
):
    experts = lax.axis_size("ep")
    per_group = experts // GROUPS
    seq_count, model_width = normed_moe.shape
    capacity = max(2, 4 * seq_count // experts)
    group_rows = -(-min(seq_count, per_group * capacity // TOP_K) // 8) * 8
    peer_rows = GROUPS * capacity
    width = model_width // CHUNKS
    hidden_width = expert_gate.shape[-1]
    slots = GROUPS * group_rows
    my_group = lax.axis_index("ep") // per_group
    expert_ids = expert_group[:, None] * per_group + expert_inner
    expert_slot = earlier_equal(expert_ids.reshape(-1)).reshape(seq_count, TOP_K)
    row_code = expert_inner * peer_rows + my_group * capacity + expert_slot + 1
    group_slot = expert_group * group_rows + earlier_equal(expert_group)
    slot_ids = jnp.arange(slots, dtype=jnp.int32)
    place = (slot_ids[:, None] == group_slot[None, :]).astype(jnp.bfloat16)
    collect = (group_slot[:, None] == slot_ids[None, :]).astype(jnp.bfloat16)
    high = lax.reduce_precision(route_weights, 8, 7)
    low = route_weights - high
    token_meta = jnp.concatenate(
        [row_code.astype(jnp.float32), high[:, :1], low[:, :1], high[:, 1:], low[:, 1:]], axis=1
    )
    token_meta = jnp.pad(token_meta, ((0, 0), (0, 128 - token_meta.shape[1]))).astype(jnp.bfloat16)
    vmem = pl.BlockSpec(memory_space=pltpu.VMEM)
    hbm = pl.BlockSpec(memory_space=pl.ANY)
    bf16 = jnp.bfloat16
    column_buffer = pltpu.VMEM((CHUNKS, GROUPS, group_rows, width), bf16)
    plane_buffer = pltpu.VMEM((CHUNKS, per_group, peer_rows, width), bf16)
    meta_buffer = pltpu.VMEM((GROUPS, group_rows, 128), bf16)
    dma = pltpu.SemaphoreType.DMA

    def kernel(*refs):
        exchange_kernel(per_group, *refs)

    return pl.pallas_call(
        kernel,
        name="experts",
        out_shape=jax.ShapeDtypeStruct((seq_count, model_width), bf16),
        in_specs=[vmem] * 5 + [hbm] * 3,
        out_specs=vmem,
        scratch_shapes=[
            pltpu.VMEM((model_width, hidden_width), bf16),
            pltpu.VMEM((model_width, hidden_width), bf16),
            pltpu.VMEM((hidden_width, model_width), bf16),
            meta_buffer,
            meta_buffer,
            column_buffer,
            column_buffer,
            plane_buffer,
            plane_buffer,
            plane_buffer,
            plane_buffer,
            column_buffer,
            column_buffer,
            dma((3,)),
            dma((2, GROUPS)),
            dma((2, CHUNKS, GROUPS)),
            dma((2, CHUNKS, per_group)),
            dma((2, CHUNKS, per_group)),
            dma((2, CHUNKS, GROUPS)),
        ],
        compiler_params=pltpu.CompilerParams(
            collective_id=0, has_side_effects=True, vmem_limit_bytes=48 * 1024 * 1024
        ),
    )(normed_moe, mixed_tokens, place, collect, token_meta, expert_gate, expert_up, expert_down)


def local(
    tokens,
    history_length,
    norm_gain,
    w_query,
    w_key,
    w_value,
    w_gate,
    decay_rate,
    state,
    head_gain,
    w_out,
    moe_gain,
    route_weights,
    expert_group,
    expert_inner,
    expert_gate,
    expert_up,
    expert_down,
):
    mixed_tokens, normed_moe, new_state = retention_step(
        tokens,
        history_length,
        norm_gain,
        w_query,
        w_key,
        w_value,
        w_gate,
        decay_rate,
        state,
        head_gain,
        w_out,
        moe_gain,
    )
    output = routed_experts(
        mixed_tokens,
        normed_moe,
        route_weights,
        expert_group,
        expert_inner,
        expert_gate[0],
        expert_up[0],
        expert_down[0],
    )
    return (output, new_state)


def solution(mesh):
    return jax.shard_map(
        local,
        mesh=mesh,
        in_specs=(
            P("ep", None),
            P("ep"),
            P(),
            P(),
            P(),
            P(),
            P(),
            P(),
            P("ep", None, None, None),
            P(),
            P(),
            P(),
            P("ep", None),
            P("ep"),
            P("ep", None),
            P("ep", None, None),
            P("ep", None, None),
            P("ep", None, None),
        ),
        out_specs=(P("ep", None), P("ep", None, None, None)),
        check_vma=False,
    )
```

```python
import jax
import jax.numpy as jnp
from jax import lax
from jax.experimental import pallas as pl
from jax.experimental.pallas import tpu as pltpu
from jax.sharding import PartitionSpec as P

GROUPS = 4
TOP_K = 2


epsilon = 1e-06


BLOCK = 8


def dot(a, b):
    return jnp.dot(a, b, preferred_element_type=jnp.float32)


def rms(values, gains):
    mean = jnp.mean(values * values, axis=-1, keepdims=True)
    return values * lax.rsqrt(mean + epsilon) * gains


def retention_kernel(
    tokens,
    cosine,
    sine,
    norm_gain,
    decay_rate,
    head_gain,
    moe_gain,
    query_hbm,
    key_hbm,
    value_hbm,
    gate_hbm,
    out_hbm,
    state_hbm,
    mixed_out,
    normed_out,
    new_state_hbm,
    query_w,
    key_w,
    value_w,
    gate_w,
    out_w,
    state,
    query_columns,
    key_columns,
    value_heads,
    reading,
    weight_sem,
    in_sem,
    out_sem,
):
    seq_count = tokens.shape[0]
    heads, head_width = state.shape[1], state.shape[-1]
    half = head_width // 2
    blocks = seq_count // BLOCK
    weight_copies = [
        pltpu.make_async_copy(source, target, weight_sem.at[index])
        for index, (source, target) in enumerate(
            (
                (key_hbm, key_w),
                (query_hbm, query_w),
                (value_hbm, value_w),
                (gate_hbm, gate_w),
                (out_hbm, out_w),
            )
        )
    ]

    def state_in(block):
        rows = pl.ds(block * BLOCK, BLOCK)
        return pltpu.make_async_copy(state_hbm.at[rows], state.at[rows], in_sem.at[block])

    def state_out(block):
        rows = pl.ds(block * BLOCK, BLOCK)
        return pltpu.make_async_copy(state.at[rows], new_state_hbm.at[rows], out_sem.at[block])

    for copy in weight_copies[:3]:
        copy.start()
    for block in range(blocks):
        state_in(block).start()
    for copy in weight_copies[3:]:
        copy.start()
    inputs = tokens[...].astype(jnp.float32)
    normed = rms(inputs, norm_gain[...]).astype(jnp.bfloat16)
    cosines = jnp.concatenate([cosine[...]] * (2 * heads), axis=1)
    sines = jnp.concatenate([-sine[...], sine[...]] * heads, axis=1)
    lane = lax.broadcasted_iota(jnp.int32, cosines.shape, 1)
    leading = lax.rem(lane, head_width) < half

    def rounded(weights):
        return dot(normed, weights[...]).astype(jnp.bfloat16).astype(jnp.float32)

    def rotated(values):
        partner = jnp.where(
            leading, jnp.roll(values, -half, axis=1), jnp.roll(values, half, axis=1)
        )
        return values * cosines + partner * sines

    weight_copies[0].wait()
    keys = rotated(rounded(key_w)) * head_width ** (-0.5)
    weight_copies[1].wait()
    queries = rotated(rounded(query_w))
    for block in range(blocks):
        rows = slice(block * BLOCK, (block + 1) * BLOCK)
        key_columns[block] = keys[rows].T
        query_columns[block] = queries[rows].T
    weight_copies[2].wait()
    values = rounded(value_w)
    for head in range(heads):
        value_heads[head] = values[:, head * head_width : (head + 1) * head_width]
    retain = [
        jnp.exp(jnp.full((1, head_width), -decay_rate[head], jnp.float32)) for head in range(heads)
    ]

    def update(block, carry):
        state_in(block).wait()
        for head in range(heads):
            span = slice(head * head_width, (head + 1) * head_width)
            block_values = value_heads[head, pl.ds(block * BLOCK, BLOCK), :]
            block_keys = key_columns[block, span, :]
            block_queries = query_columns[block, span, :]
            rows = []
            for index in range(BLOCK):
                sequence = block * BLOCK + index
                fresh = (
                    retain[head] * state[sequence, head]
                    + block_keys[:, index : index + 1] * block_values[index : index + 1, :]
                )
                state[sequence, head] = fresh
                rows.append(
                    jnp.sum(block_queries[:, index : index + 1] * fresh, axis=0, keepdims=True)
                )
            reading[head, pl.ds(block * BLOCK, BLOCK), :] = jnp.concatenate(rows, axis=0)
        state_out(block).start()
        return carry

    lax.fori_loop(0, blocks, update, 0)
    weight_copies[3].wait()
    gating = rounded(gate_w)
    read = jnp.concatenate(
        [
            rms(
                reading[head],
                head_gain[:, head * head_width : (head + 1) * head_width],
            )
            for head in range(heads)
        ],
        axis=1,
    )
    mixed_heads = (read * jax.nn.silu(gating)).astype(jnp.bfloat16)
    weight_copies[4].wait()
    mixed_tokens = (inputs + dot(mixed_heads, out_w[...])).astype(jnp.bfloat16)
    mixed_out[...] = mixed_tokens
    normed_out[...] = rms(mixed_tokens.astype(jnp.float32), moe_gain[...]).astype(jnp.bfloat16)
    for block in range(blocks):
        state_out(block).wait()


def retention_step(
    tokens,
    history_length,
    norm_gain,
    w_query,
    w_key,
    w_value,
    w_gate,
    decay_rate,
    state,
    head_gain,
    w_out,
    moe_gain,
):
    heads = decay_rate.shape[0]
    seq_count, model_width = tokens.shape
    head_width = state.shape[-1]
    half = head_width // 2
    blocks = seq_count // BLOCK
    inverse = 10000.0 ** (-jnp.arange(half, dtype=jnp.float32) / half)
    angles = history_length.astype(jnp.float32)[:, None] * inverse[None, :]
    vmem = pl.BlockSpec(memory_space=pltpu.VMEM)
    smem = pl.BlockSpec(memory_space=pltpu.SMEM)
    hbm = pl.BlockSpec(memory_space=pl.ANY)
    dma = pltpu.SemaphoreType.DMA
    f32 = jnp.float32
    row_shape = jax.ShapeDtypeStruct((seq_count, model_width), jnp.bfloat16)
    return pl.pallas_call(
        retention_kernel,
        name="retention",
        out_shape=(row_shape, row_shape, jax.ShapeDtypeStruct(state.shape, f32)),
        in_specs=[vmem] * 4 + [smem] + [vmem] * 2 + [hbm] * 6,
        out_specs=(vmem, vmem, hbm),
        scratch_shapes=[pltpu.VMEM(w_query.shape, jnp.bfloat16)] * 4
        + [
            pltpu.VMEM(w_out.shape, jnp.bfloat16),
            pltpu.VMEM(state.shape, f32),
            pltpu.VMEM((blocks, heads * head_width, BLOCK), f32),
            pltpu.VMEM((blocks, heads * head_width, BLOCK), f32),
            pltpu.VMEM((heads, seq_count, head_width), f32),
            pltpu.VMEM((heads, seq_count, head_width), f32),
            dma((5,)),
            dma((blocks,)),
            dma((blocks,)),
        ],
        compiler_params=pltpu.CompilerParams(vmem_limit_bytes=60 * 1024 * 1024),
    )(
        tokens,
        jnp.cos(angles),
        jnp.sin(angles),
        norm_gain.reshape(1, -1),
        decay_rate,
        head_gain.reshape(1, -1),
        moe_gain.reshape(1, -1),
        w_query,
        w_key,
        w_value,
        w_gate,
        w_out,
        state,
    )


MESH = pl.DeviceIdType.MESH
CHUNKS = 4


def exchange_kernel(
    per_group,
    normed,
    mixed,
    expert_group,
    expert_inner,
    route_weights,
    gate_hbm,
    up_hbm,
    down_hbm,
    out,
    gate_w,
    up_w,
    down_w,
    meta_send,
    meta_recv,
    zsend,
    zrecv,
    dsend,
    drecv,
    osend,
    orecv,
    csend,
    crecv,
    load_sem,
    meta_sems,
    z_sems,
    d_sems,
    o_sems,
    c_sems,
):
    device = lax.axis_index("ep")
    group = device // per_group
    inner = device % per_group
    width = zsend.shape[-1]
    group_rows = zsend.shape[2]
    peer_rows = dsend.shape[2]
    slots = GROUPS * group_rows
    rows = per_group * peer_rows

    def column_peer(step):
        other = lax.rem(group + step, GROUPS)
        return other, other * per_group + inner

    def plane_peer(step):
        other = lax.rem(inner + step, per_group)
        return other, group * per_group + other

    def column_copy(source, target, sems, chunk, step):
        other, peer = column_peer(step)
        return pltpu.make_async_remote_copy(
            src_ref=source.at[chunk, other],
            dst_ref=target.at[chunk, group],
            send_sem=sems.at[0, chunk, step],
            recv_sem=sems.at[1, chunk, step],
            device_id=(peer,),
            device_id_type=MESH,
        )

    def plane_copy(source, target, sems, chunk, step):
        other, peer = plane_peer(step)
        return pltpu.make_async_remote_copy(
            src_ref=source.at[chunk, other],
            dst_ref=target.at[chunk, inner],
            send_sem=sems.at[0, chunk, step],
            recv_sem=sems.at[1, chunk, step],
            device_id=(peer,),
            device_id_type=MESH,
        )

    def meta_copy(step):
        other, peer = column_peer(step)
        return pltpu.make_async_remote_copy(
            src_ref=meta_send.at[other],
            dst_ref=meta_recv.at[group],
            send_sem=meta_sems.at[0, step],
            recv_sem=meta_sems.at[1, step],
            device_id=(peer,),
            device_id_type=MESH,
        )

    def each_column(act):
        for step in (2, 1, 3):
            act(step)

    def each_plane(act):
        def body(step, carry):
            act(step)
            return carry

        lax.fori_loop(1, per_group, body, 0)

    loads = [
        pltpu.make_async_copy(source, target, load_sem.at[place_index])
        for place_index, (source, target) in enumerate(
            ((gate_hbm, gate_w), (up_hbm, up_w), (down_hbm, down_w))
        )
    ]
    for load in loads:
        load.start()
    barrier = pltpu.get_barrier_semaphore()

    def greet_column(step):
        pl.semaphore_signal(barrier, inc=1, device_id=(column_peer(step)[1],), device_id_type=MESH)

    def greet_plane(step):
        pl.semaphore_signal(barrier, inc=1, device_id=(plane_peer(step)[1],), device_id_type=MESH)

    each_column(greet_column)
    each_plane(greet_plane)
    seq_count = normed.shape[0]
    group_row = expert_group[...].astype(jnp.float32)
    inner_rows = [expert_inner[choice : choice + 1, :].astype(jnp.float32) for choice in (0, 1)]
    square = (seq_count, seq_count)
    above = lax.broadcasted_iota(jnp.int32, square, 0)
    across = lax.broadcasted_iota(jnp.int32, square, 1)

    def column(row):
        return jnp.sum(jnp.where(above == across, row, 0.0), axis=1, keepdims=True)

    def earlier(columns, row):
        matched = sum((values == row).astype(jnp.float32) for values in columns)
        return jnp.sum(jnp.where(above < across, matched, 0.0), axis=0, keepdims=True)

    group_slot = group_row * group_rows + earlier([column(group_row)], group_row)
    expert_rows = [group_row * per_group + row for row in inner_rows]
    expert_columns = [column(row) for row in expert_rows]
    capacity = peer_rows // GROUPS
    own_rows = (group * capacity + 1).astype(jnp.float32)
    lanes = []
    for choice in (0, 1):
        slot = earlier(expert_columns, expert_rows[choice])
        lanes.append(column(inner_rows[choice] * peer_rows + own_rows + slot))
    for choice in (0, 1):
        weight = column(route_weights[choice : choice + 1, :])
        high = weight.astype(jnp.bfloat16).astype(jnp.float32)
        lanes += [high, weight - high]
    lane = lax.broadcasted_iota(jnp.int32, (seq_count, meta_send.shape[-1]), 1)
    token_meta = jnp.zeros(lane.shape, jnp.float32)
    for index, value in enumerate(lanes):
        token_meta = jnp.where(lane == index, value, token_meta)
    slot_above = lax.broadcasted_iota(jnp.int32, (slots, seq_count), 0).astype(jnp.float32)
    slot_across = lax.broadcasted_iota(jnp.int32, (seq_count, slots), 1).astype(jnp.float32)
    placing = (slot_above == group_slot).astype(jnp.float32).astype(jnp.bfloat16)
    collecting = (slot_across == column(group_slot)).astype(jnp.float32).astype(jnp.bfloat16)
    meta = dot(placing, token_meta.astype(jnp.bfloat16)).astype(jnp.bfloat16)
    meta_send[...] = meta.reshape(meta_send.shape)
    for chunk in range(CHUNKS):
        columns = slice(chunk * width, (chunk + 1) * width)
        block = dot(placing, normed[:, columns]).astype(jnp.bfloat16)
        zsend[chunk] = block.reshape(zsend.shape[1:])
    pl.semaphore_wait(barrier, GROUPS - 1 + per_group - 1)
    each_column(lambda step: meta_copy(step).start())
    for chunk in range(CHUNKS):
        each_column(lambda step: column_copy(zsend, zrecv, z_sems, chunk, step).start())
    meta_recv[group] = meta_send[group]
    for chunk in range(CHUNKS):
        zrecv[chunk, group] = zsend[chunk, group]
    each_column(lambda step: meta_copy(step).wait_recv())
    meta = meta_recv[...].reshape(slots, meta_recv.shape[-1]).astype(jnp.float32)
    row_ids = lax.broadcasted_iota(jnp.int32, (slots, rows), 1).astype(jnp.float32) + 1.0
    first = (row_ids == meta[:, 0:1]).astype(jnp.float32)
    second = (row_ids == meta[:, 1:2]).astype(jnp.float32)
    spread = (first + second).astype(jnp.bfloat16)
    weights = first * (meta[:, 2:3] + meta[:, 3:4]) + second * (meta[:, 4:5] + meta[:, 5:6])
    weights_high = weights.astype(jnp.bfloat16)
    weights_low = (weights - weights_high.astype(jnp.float32)).astype(jnp.bfloat16)
    for chunk in range(CHUNKS):
        each_column(lambda step: column_copy(zsend, zrecv, z_sems, chunk, step).wait_recv())
        block = lax.dot_general(
            spread,
            zrecv[chunk].reshape(slots, width),
            (((0,), (0,)), ((), ())),
            preferred_element_type=jnp.float32,
        ).astype(jnp.bfloat16)
        dsend[chunk] = block.reshape(dsend.shape[1:])
        each_plane(lambda step: plane_copy(dsend, drecv, d_sems, chunk, step).start())
        drecv[chunk, inner] = dsend[chunk, inner]
    loads[0].wait()
    loads[1].wait()
    loads[2].wait()
    gate_part = jnp.zeros((rows, gate_w.shape[1]), jnp.float32)
    up_part = jnp.zeros((rows, gate_w.shape[1]), jnp.float32)
    for chunk in range(CHUNKS):
        columns = slice(chunk * width, (chunk + 1) * width)
        each_plane(lambda step: plane_copy(dsend, drecv, d_sems, chunk, step).wait_recv())
        block = drecv[chunk].reshape(rows, width)
        gate_part += dot(block, gate_w[columns, :])
        up_part += dot(block, up_w[columns, :])
    hidden = (jax.nn.silu(gate_part) * up_part).astype(jnp.bfloat16)
    for chunk in range(CHUNKS):
        columns = slice(chunk * width, (chunk + 1) * width)
        block = dot(hidden, down_w[:, columns]).astype(jnp.bfloat16)
        osend[chunk] = block.reshape(osend.shape[1:])
        each_plane(lambda step: plane_copy(osend, orecv, o_sems, chunk, step).start())
        orecv[chunk, inner] = osend[chunk, inner]
    for chunk in range(CHUNKS):
        each_plane(lambda step: plane_copy(osend, orecv, o_sems, chunk, step).wait_recv())
        block = orecv[chunk].reshape(rows, width)
        block = (dot(weights_high, block) + dot(weights_low, block)).astype(jnp.bfloat16)
        csend[chunk] = block.reshape(csend.shape[1:])
        each_column(lambda step: column_copy(csend, crecv, c_sems, chunk, step).start())
        crecv[chunk, group] = csend[chunk, group]
    for chunk in range(CHUNKS):
        columns = slice(chunk * width, (chunk + 1) * width)
        each_column(lambda step: column_copy(csend, crecv, c_sems, chunk, step).wait_recv())
        block = dot(collecting, crecv[chunk].reshape(slots, width))
        out[:, columns] = (mixed[:, columns].astype(jnp.float32) + block).astype(jnp.bfloat16)
    each_column(lambda step: meta_copy(step).wait_send())

    def drain(chunk, carry):
        each_column(lambda step: column_copy(zsend, zrecv, z_sems, chunk, step).wait_send())
        each_column(lambda step: column_copy(csend, crecv, c_sems, chunk, step).wait_send())
        each_plane(lambda step: plane_copy(dsend, drecv, d_sems, chunk, step).wait_send())
        each_plane(lambda step: plane_copy(osend, orecv, o_sems, chunk, step).wait_send())
        return carry

    lax.fori_loop(0, CHUNKS, drain, 0)


def routed_experts(
    mixed_tokens, normed_moe, route_weights, expert_group, expert_inner, expert_gate, expert_up, expert_down
):
    experts = lax.axis_size("ep")
    per_group = experts // GROUPS
    seq_count, model_width = normed_moe.shape
    capacity = max(2, 4 * seq_count // experts)
    group_rows = -(-min(seq_count, per_group * capacity // TOP_K) // 8) * 8
    peer_rows = GROUPS * capacity
    width = model_width // CHUNKS
    hidden_width = expert_gate.shape[-1]
    slots = GROUPS * group_rows
    vmem = pl.BlockSpec(memory_space=pltpu.VMEM)
    hbm = pl.BlockSpec(memory_space=pl.ANY)
    bf16 = jnp.bfloat16
    column_buffer = pltpu.VMEM((CHUNKS, GROUPS, group_rows, width), bf16)
    plane_buffer = pltpu.VMEM((CHUNKS, per_group, peer_rows, width), bf16)
    meta_buffer = pltpu.VMEM((GROUPS, group_rows, 128), bf16)
    dma = pltpu.SemaphoreType.DMA

    def kernel(*refs):
        exchange_kernel(per_group, *refs)

    return pl.pallas_call(
        kernel,
        name="experts",
        out_shape=jax.ShapeDtypeStruct((seq_count, model_width), bf16),
        in_specs=[vmem] * 5 + [hbm] * 3,
        out_specs=vmem,
        scratch_shapes=[
            pltpu.VMEM((model_width, hidden_width), bf16),
            pltpu.VMEM((model_width, hidden_width), bf16),
            pltpu.VMEM((hidden_width, model_width), bf16),
            meta_buffer,
            meta_buffer,
            column_buffer,
            column_buffer,
            plane_buffer,
            plane_buffer,
            plane_buffer,
            plane_buffer,
            column_buffer,
            column_buffer,
            dma((3,)),
            dma((2, GROUPS)),
            dma((2, CHUNKS, GROUPS)),
            dma((2, CHUNKS, per_group)),
            dma((2, CHUNKS, per_group)),
            dma((2, CHUNKS, GROUPS)),
        ],
        compiler_params=pltpu.CompilerParams(
            collective_id=0, has_side_effects=True, vmem_limit_bytes=60 * 1024 * 1024
        ),
    )(
        normed_moe,
        mixed_tokens,
        expert_group.reshape(1, -1),
        expert_inner.T,
        route_weights.T,
        expert_gate,
        expert_up,
        expert_down,
    )


def local(
    tokens,
    history_length,
    norm_gain,
    w_query,
    w_key,
    w_value,
    w_gate,
    decay_rate,
    state,
    head_gain,
    w_out,
    moe_gain,
    route_weights,
    expert_group,
    expert_inner,
    expert_gate,
    expert_up,
    expert_down,
):
    mixed_tokens, normed_moe, new_state = retention_step(
        tokens,
        history_length,
        norm_gain,
        w_query,
        w_key,
        w_value,
        w_gate,
        decay_rate,
        state,
        head_gain,
        w_out,
        moe_gain,
    )
    output = routed_experts(
        mixed_tokens,
        normed_moe,
        route_weights,
        expert_group,
        expert_inner,
        expert_gate[0],
        expert_up[0],
        expert_down[0],
    )
    return (output, new_state)


def solution(mesh):
    return jax.shard_map(
        local,
        mesh=mesh,
        in_specs=(
            P("ep", None),
            P("ep"),
            P(),
            P(),
            P(),
            P(),
            P(),
            P(),
            P("ep", None, None, None),
            P(),
            P(),
            P(),
            P("ep", None),
            P("ep"),
            P("ep", None),
            P("ep", None, None),
            P("ep", None, None),
            P("ep", None, None),
        ),
        out_specs=(P("ep", None), P("ep", None, None, None)),
        check_vma=False,
    )
```

```python
import jax
import jax.numpy as jnp
import numpy as np
from jax import lax
from jax.experimental import pallas as pl
from jax.experimental.pallas import tpu as pltpu
from jax.sharding import PartitionSpec as P

GROUPS = 4
TOP_K = 2


epsilon = 1e-06


BLOCK = 8


def dot(a, b):
    return jnp.dot(a, b, preferred_element_type=jnp.float32)


def rms(values, gains):
    mean = jnp.mean(values * values, axis=-1, keepdims=True)
    return values * lax.rsqrt(mean + epsilon) * gains


def retention_kernel(
    tokens,
    history_length,
    inverse,
    norm_gain,
    decay_rate,
    head_gain,
    query_hbm,
    key_hbm,
    value_hbm,
    gate_hbm,
    out_hbm,
    state_hbm,
    mixed_out,
    new_state_hbm,
    query_w,
    key_w,
    value_w,
    gate_w,
    out_w,
    state,
    query_columns,
    key_columns,
    value_heads,
    reading,
    weight_sem,
    in_sem,
    out_sem,
):
    seq_count = tokens.shape[0]
    heads, head_width = state.shape[1], state.shape[-1]
    half = head_width // 2
    blocks = seq_count // BLOCK
    weight_copies = [
        pltpu.make_async_copy(source, target, weight_sem.at[index])
        for index, (source, target) in enumerate(
            (
                (key_hbm, key_w),
                (query_hbm, query_w),
                (value_hbm, value_w),
                (gate_hbm, gate_w),
                (out_hbm, out_w),
            )
        )
    ]

    def state_in(block):
        rows = pl.ds(block * BLOCK, BLOCK)
        return pltpu.make_async_copy(state_hbm.at[rows], state.at[rows], in_sem.at[block])

    def state_out(block):
        rows = pl.ds(block * BLOCK, BLOCK)
        return pltpu.make_async_copy(state.at[rows], new_state_hbm.at[rows], out_sem.at[block])

    for copy in weight_copies[:3]:
        copy.start()
    for block in range(blocks):
        state_in(block).start()
    for copy in weight_copies[3:]:
        copy.start()
    inputs = tokens[...].astype(jnp.float32)
    normed = rms(inputs, norm_gain[...]).astype(jnp.bfloat16)
    square = (seq_count, seq_count)
    above = lax.broadcasted_iota(jnp.int32, square, 0)
    across = lax.broadcasted_iota(jnp.int32, square, 1)
    places = history_length[...].astype(jnp.float32)
    places = jnp.sum(jnp.where(above == across, places, 0.0), axis=1, keepdims=True)
    angles = places * inverse[...]
    cosine, sine = jnp.cos(angles), jnp.sin(angles)
    cosines = jnp.concatenate([cosine] * (2 * heads), axis=1)
    sines = jnp.concatenate([-sine, sine] * heads, axis=1)
    lane = lax.broadcasted_iota(jnp.int32, cosines.shape, 1)
    leading = lax.rem(lane, head_width) < half

    def rounded(weights):
        return dot(normed, weights[...]).astype(jnp.bfloat16).astype(jnp.float32)

    def rotated(values):
        partner = jnp.where(
            leading, jnp.roll(values, -half, axis=1), jnp.roll(values, half, axis=1)
        )
        return values * cosines + partner * sines

    weight_copies[0].wait()
    keys = rotated(rounded(key_w)) * head_width ** (-0.5)
    weight_copies[1].wait()
    queries = rotated(rounded(query_w))
    for block in range(blocks):
        rows = slice(block * BLOCK, (block + 1) * BLOCK)
        key_columns[block] = keys[rows].T
        query_columns[block] = queries[rows].T
    weight_copies[2].wait()
    values = rounded(value_w)
    for head in range(heads):
        value_heads[head] = values[:, head * head_width : (head + 1) * head_width]
    retain = [
        jnp.exp(jnp.full((1, head_width), -decay_rate[head], jnp.float32)) for head in range(heads)
    ]

    def update(block, carry):
        state_in(block).wait()
        for head in range(heads):
            span = slice(head * head_width, (head + 1) * head_width)
            block_values = value_heads[head, pl.ds(block * BLOCK, BLOCK), :]
            block_keys = key_columns[block, span, :]
            block_queries = query_columns[block, span, :]
            rows = []
            for index in range(BLOCK):
                sequence = block * BLOCK + index
                fresh = (
                    retain[head] * state[sequence, head]
                    + block_keys[:, index : index + 1] * block_values[index : index + 1, :]
                )
                state[sequence, head] = fresh
                rows.append(
                    jnp.sum(block_queries[:, index : index + 1] * fresh, axis=0, keepdims=True)
                )
            reading[head, pl.ds(block * BLOCK, BLOCK), :] = jnp.concatenate(rows, axis=0)
        state_out(block).start()
        return carry

    lax.fori_loop(0, blocks, update, 0)
    weight_copies[3].wait()
    gating = rounded(gate_w)
    read = jnp.concatenate(
        [
            rms(
                reading[head],
                head_gain[:, head * head_width : (head + 1) * head_width],
            )
            for head in range(heads)
        ],
        axis=1,
    )
    mixed_heads = (read * jax.nn.silu(gating)).astype(jnp.bfloat16)
    weight_copies[4].wait()
    mixed_out[...] = (inputs + dot(mixed_heads, out_w[...])).astype(jnp.bfloat16)
    for block in range(blocks):
        state_out(block).wait()


def retention_step(
    tokens,
    history_length,
    norm_gain,
    w_query,
    w_key,
    w_value,
    w_gate,
    decay_rate,
    state,
    head_gain,
    w_out,
):
    heads = decay_rate.shape[0]
    seq_count, model_width = tokens.shape
    head_width = state.shape[-1]
    half = head_width // 2
    blocks = seq_count // BLOCK
    inverse = (10000.0 ** (-np.arange(half) / half)).astype(np.float32)
    vmem = pl.BlockSpec(memory_space=pltpu.VMEM)
    smem = pl.BlockSpec(memory_space=pltpu.SMEM)
    hbm = pl.BlockSpec(memory_space=pl.ANY)
    dma = pltpu.SemaphoreType.DMA
    f32 = jnp.float32
    row_shape = jax.ShapeDtypeStruct((seq_count, model_width), jnp.bfloat16)
    return pl.pallas_call(
        retention_kernel,
        name="retention",
        out_shape=(row_shape, jax.ShapeDtypeStruct(state.shape, f32)),
        in_specs=[vmem] * 4 + [smem, vmem] + [hbm] * 6,
        out_specs=(vmem, hbm),
        scratch_shapes=[pltpu.VMEM(w_query.shape, jnp.bfloat16)] * 4
        + [
            pltpu.VMEM(w_out.shape, jnp.bfloat16),
            pltpu.VMEM(state.shape, f32),
            pltpu.VMEM((blocks, heads * head_width, BLOCK), f32),
            pltpu.VMEM((blocks, heads * head_width, BLOCK), f32),
            pltpu.VMEM((heads, seq_count, head_width), f32),
            pltpu.VMEM((heads, seq_count, head_width), f32),
            dma((5,)),
            dma((blocks,)),
            dma((blocks,)),
        ],
        compiler_params=pltpu.CompilerParams(vmem_limit_bytes=60 * 1024 * 1024),
    )(
        tokens,
        history_length.reshape(1, -1),
        inverse.reshape(1, -1),
        norm_gain.reshape(1, -1),
        decay_rate,
        head_gain.reshape(1, -1),
        w_query,
        w_key,
        w_value,
        w_gate,
        w_out,
        state,
    )


MESH = pl.DeviceIdType.MESH
STAGES = GROUPS


def exchange_kernel(
    per_group,
    moe_gain,
    mixed,
    expert_group,
    expert_inner,
    route_weights,
    gate_hbm,
    up_hbm,
    down_hbm,
    out,
    gate_w,
    up_w,
    down_w,
    meta_send,
    meta_recv,
    zsend,
    zrecv,
    dsend,
    drecv,
    osend,
    orecv,
    csend,
    crecv,
    load_sem,
    meta_sems,
    z_sems,
    d_sems,
    o_sems,
    c_sems,
):
    device = lax.axis_index("ep")
    group = device // per_group
    inner = device % per_group
    width = zsend.shape[-1]
    group_rows = zsend.shape[1]
    peer_rows = dsend.shape[2]
    slots = GROUPS * group_rows
    rows = per_group * peer_rows

    def column_peer(step):
        other = lax.rem(group + step, GROUPS)
        return other, other * per_group + inner

    def plane_peer(step):
        other = lax.rem(inner + step, per_group)
        return other, group * per_group + other

    def send_out(step):
        other, peer = column_peer(step)
        return pltpu.make_async_remote_copy(
            src_ref=zsend.at[other],
            dst_ref=zrecv.at[step],
            send_sem=z_sems.at[0, step],
            recv_sem=z_sems.at[1, step],
            device_id=(peer,),
            device_id_type=MESH,
        )

    def send_home(step):
        home = lax.rem(group + GROUPS - step, GROUPS)
        return pltpu.make_async_remote_copy(
            src_ref=csend.at[step],
            dst_ref=crecv.at[group],
            send_sem=c_sems.at[0, step],
            recv_sem=c_sems.at[1, step],
            device_id=(home * per_group + inner,),
            device_id_type=MESH,
        )

    def plane_copy(source, target, sems, stage, step):
        other, peer = plane_peer(step)
        return pltpu.make_async_remote_copy(
            src_ref=source.at[stage, other],
            dst_ref=target.at[stage, inner],
            send_sem=sems.at[0, stage, step],
            recv_sem=sems.at[1, stage, step],
            device_id=(peer,),
            device_id_type=MESH,
        )

    def meta_copy(step):
        other, peer = column_peer(step)
        return pltpu.make_async_remote_copy(
            src_ref=meta_send.at[other],
            dst_ref=meta_recv.at[step],
            send_sem=meta_sems.at[0, step],
            recv_sem=meta_sems.at[1, step],
            device_id=(peer,),
            device_id_type=MESH,
        )

    def each_column(act):
        for step in range(1, GROUPS):
            act(step)

    def each_plane(act):
        def body(step, carry):
            act(step)
            return carry

        lax.fori_loop(1, per_group, body, 0)

    loads = [
        pltpu.make_async_copy(source, target, load_sem.at[place_index])
        for place_index, (source, target) in enumerate(
            ((gate_hbm, gate_w), (up_hbm, up_w), (down_hbm, down_w))
        )
    ]
    for load in loads:
        load.start()
    barrier = pltpu.get_barrier_semaphore()

    def greet_column(step):
        pl.semaphore_signal(barrier, inc=1, device_id=(column_peer(step)[1],), device_id_type=MESH)

    def greet_plane(step):
        pl.semaphore_signal(barrier, inc=1, device_id=(plane_peer(step)[1],), device_id_type=MESH)

    each_column(greet_column)
    each_plane(greet_plane)
    seq_count = mixed.shape[0]
    normed = rms(mixed[...].astype(jnp.float32), moe_gain[...]).astype(jnp.bfloat16)
    group_row = expert_group[...].astype(jnp.float32)
    inner_rows = [expert_inner[choice : choice + 1, :].astype(jnp.float32) for choice in (0, 1)]
    square = (seq_count, seq_count)
    above = lax.broadcasted_iota(jnp.int32, square, 0)
    across = lax.broadcasted_iota(jnp.int32, square, 1)

    def column(row):
        return jnp.sum(jnp.where(above == across, row, 0.0), axis=1, keepdims=True)

    def earlier(columns, row):
        matched = sum((values == row).astype(jnp.float32) for values in columns)
        return jnp.sum(jnp.where(above < across, matched, 0.0), axis=0, keepdims=True)

    group_slot = group_row * group_rows + earlier([column(group_row)], group_row)
    expert_rows = [group_row * per_group + row for row in inner_rows]
    expert_columns = [column(row) for row in expert_rows]
    lanes = []
    for choice in (0, 1):
        slot = earlier(expert_columns, expert_rows[choice])
        lanes.append(column(inner_rows[choice] * peer_rows + slot + 1.0))
    for choice in (0, 1):
        weight = column(route_weights[choice : choice + 1, :])
        high = weight.astype(jnp.bfloat16).astype(jnp.float32)
        lanes += [high, weight - high]
    lane = lax.broadcasted_iota(jnp.int32, (seq_count, meta_send.shape[-1]), 1)
    token_meta = jnp.zeros(lane.shape, jnp.float32)
    for index, value in enumerate(lanes):
        token_meta = jnp.where(lane == index, value, token_meta)
    slot_above = lax.broadcasted_iota(jnp.int32, (slots, seq_count), 0).astype(jnp.float32)
    slot_across = lax.broadcasted_iota(jnp.int32, (seq_count, slots), 1).astype(jnp.float32)
    placing = (slot_above == group_slot).astype(jnp.float32).astype(jnp.bfloat16)
    collecting = (slot_across == column(group_slot)).astype(jnp.float32).astype(jnp.bfloat16)
    meta = dot(placing, token_meta.astype(jnp.bfloat16)).astype(jnp.bfloat16)
    meta_send[...] = meta.reshape(meta_send.shape)
    zsend[...] = dot(placing, normed).astype(jnp.bfloat16).reshape(zsend.shape)
    pl.semaphore_wait(barrier, GROUPS - 1 + per_group - 1)
    each_column(lambda step: meta_copy(step).start())
    each_column(lambda step: send_out(step).start())
    meta_recv[0] = meta_send[group]
    zrecv[0] = zsend[group]
    weights_of = {}

    def spread_rows(stage):
        if stage:
            meta_copy(stage).wait_recv()
        meta = meta_recv[stage].astype(jnp.float32)
        row_ids = lax.broadcasted_iota(jnp.int32, (group_rows, rows), 1).astype(jnp.float32) + 1.0
        first = (row_ids == meta[:, 0:1]).astype(jnp.float32)
        second = (row_ids == meta[:, 1:2]).astype(jnp.float32)
        weights = first * (meta[:, 2:3] + meta[:, 3:4]) + second * (meta[:, 4:5] + meta[:, 5:6])
        high = weights.astype(jnp.bfloat16)
        weights_of[stage] = (high, (weights - high.astype(jnp.float32)).astype(jnp.bfloat16))
        if stage:
            send_out(stage).wait_recv()
        block = lax.dot_general(
            (first + second).astype(jnp.bfloat16),
            zrecv[stage],
            (((0,), (0,)), ((), ())),
            preferred_element_type=jnp.float32,
        ).astype(jnp.bfloat16)
        dsend[stage] = block.reshape(dsend.shape[1:])
        each_plane(lambda step: plane_copy(dsend, drecv, d_sems, stage, step).start())
        drecv[stage, inner] = dsend[stage, inner]

    def run_expert(stage):
        each_plane(lambda step: plane_copy(dsend, drecv, d_sems, stage, step).wait_recv())
        if stage == 0:
            for load in loads:
                load.wait()
        block = drecv[stage].reshape(rows, width)
        hidden = jax.nn.silu(dot(block, gate_w[...])) * dot(block, up_w[...])
        block = dot(hidden.astype(jnp.bfloat16), down_w[...]).astype(jnp.bfloat16)
        osend[stage] = block.reshape(osend.shape[1:])
        each_plane(lambda step: plane_copy(osend, orecv, o_sems, stage, step).start())
        orecv[stage, inner] = osend[stage, inner]

    def combine(stage):
        each_plane(lambda step: plane_copy(osend, orecv, o_sems, stage, step).wait_recv())
        block = orecv[stage].reshape(rows, width)
        high, low = weights_of[stage]
        csend[stage] = (dot(high, block) + dot(low, block)).astype(jnp.bfloat16)
        if stage:
            send_home(stage).start()
        else:
            crecv[group] = csend[0]

    spread_rows(0)
    spread_rows(1)
    run_expert(0)
    spread_rows(2)
    run_expert(1)
    spread_rows(3)
    combine(0)
    run_expert(2)
    combine(1)
    run_expert(3)
    combine(2)
    combine(3)
    each_column(lambda step: send_home(step).wait_recv())
    block = dot(collecting, crecv[...].reshape(slots, width))
    out[...] = (mixed[...].astype(jnp.float32) + block).astype(jnp.bfloat16)
    each_column(lambda step: meta_copy(step).wait_send())
    each_column(lambda step: send_out(step).wait_send())
    each_column(lambda step: send_home(step).wait_send())

    def drain(stage, carry):
        each_plane(lambda step: plane_copy(dsend, drecv, d_sems, stage, step).wait_send())
        each_plane(lambda step: plane_copy(osend, orecv, o_sems, stage, step).wait_send())
        return carry

    lax.fori_loop(0, STAGES, drain, 0)


def routed_experts(
    mixed_tokens, moe_gain, route_weights, expert_group, expert_inner, expert_gate, expert_up, expert_down
):
    experts = lax.axis_size("ep")
    per_group = experts // GROUPS
    seq_count, model_width = mixed_tokens.shape
    capacity = max(2, 4 * seq_count // experts)
    group_rows = -(-min(seq_count, per_group * capacity // TOP_K) // 8) * 8
    peer_rows = -(-capacity // 8) * 8
    hidden_width = expert_gate.shape[-1]
    vmem = pl.BlockSpec(memory_space=pltpu.VMEM)
    hbm = pl.BlockSpec(memory_space=pl.ANY)
    bf16 = jnp.bfloat16
    column_buffer = pltpu.VMEM((GROUPS, group_rows, model_width), bf16)
    plane_buffer = pltpu.VMEM((STAGES, per_group, peer_rows, model_width), bf16)
    meta_buffer = pltpu.VMEM((GROUPS, group_rows, 128), bf16)
    dma = pltpu.SemaphoreType.DMA

    def kernel(*refs):
        exchange_kernel(per_group, *refs)

    return pl.pallas_call(
        kernel,
        name="experts",
        out_shape=jax.ShapeDtypeStruct((seq_count, model_width), bf16),
        in_specs=[vmem] * 5 + [hbm] * 3,
        out_specs=vmem,
        scratch_shapes=[
            pltpu.VMEM((model_width, hidden_width), bf16),
            pltpu.VMEM((model_width, hidden_width), bf16),
            pltpu.VMEM((hidden_width, model_width), bf16),
            meta_buffer,
            meta_buffer,
            column_buffer,
            column_buffer,
            plane_buffer,
            plane_buffer,
            plane_buffer,
            plane_buffer,
            column_buffer,
            column_buffer,
            dma((3,)),
            dma((2, GROUPS)),
            dma((2, STAGES)),
            dma((2, STAGES, per_group)),
            dma((2, STAGES, per_group)),
            dma((2, STAGES)),
        ],
        compiler_params=pltpu.CompilerParams(
            collective_id=0,
            has_side_effects=True,
            vmem_limit_bytes=(16 + 20 * per_group // 32 * 2) * 1024 * 1024,
        ),
    )(
        moe_gain.reshape(1, -1),
        mixed_tokens,
        expert_group.reshape(1, -1),
        expert_inner.T,
        route_weights.T,
        expert_gate,
        expert_up,
        expert_down,
    )


def local(
    tokens,
    history_length,
    norm_gain,
    w_query,
    w_key,
    w_value,
    w_gate,
    decay_rate,
    state,
    head_gain,
    w_out,
    moe_gain,
    route_weights,
    expert_group,
    expert_inner,
    expert_gate,
    expert_up,
    expert_down,
):
    mixed_tokens, new_state = retention_step(
        tokens,
        history_length,
        norm_gain,
        w_query,
        w_key,
        w_value,
        w_gate,
        decay_rate,
        state,
        head_gain,
        w_out,
    )
    output = routed_experts(
        mixed_tokens,
        moe_gain,
        route_weights,
        expert_group,
        expert_inner,
        expert_gate[0],
        expert_up[0],
        expert_down[0],
    )
    return (output, new_state)


def solution(mesh):
    return jax.shard_map(
        local,
        mesh=mesh,
        in_specs=(
            P("ep", None),
            P("ep"),
            P(),
            P(),
            P(),
            P(),
            P(),
            P(),
            P("ep", None, None, None),
            P(),
            P(),
            P(),
            P("ep", None),
            P("ep"),
            P("ep", None),
            P("ep", None, None),
            P("ep", None, None),
            P("ep", None, None),
        ),
        out_specs=(P("ep", None), P("ep", None, None, None)),
        check_vma=False,
    )
```
